32 devices in a mesh: fs: 8 (over z, x), tp: 4 (over y, core).
Axes of the slice: x: 2, y: 2, z: 4, core: 2. Of those that a mesh axis runs over, the one named last changes fastest.
Arguments:
- tokens: bfloat16 [4096, 2048], P('fs', 'tp'), may hold values from -6 to 6
- pre_gain: float32 [2048], replicated, may hold values from 0.1 to 1.9
- pre_gate: float32 [2048, 2816], P('fs', 'tp'), may hold values from -0.125 to 0.125
- pre_up: float32 [2048, 2816], P('fs', 'tp'), may hold values from -0.125 to 0.125
- pre_down: float32 [2816, 2048], P('fs', 'tp'), may hold values from -0.109375 to 0.109375
- mix_gain: float32 [2048], replicated, may hold values from 0.1 to 1.9
- branch_proj: float32 [2048, 1024], P('fs', 'tp'), may hold values from -0.125 to 0.125
- gate_proj: float32 [2048, 1024], P('fs', 'tp'), may hold values from -0.125 to 0.125
- conv_taps: float32 [4, 1024], P(None, 'tp'), may hold values from -3 to 3
- retain_blocks: float32 [16, 64, 64], P('tp'), may hold values from -0.75 to 0.75
- admit_blocks: float32 [16, 64, 64], P('tp'), may hold values from -0.75 to 0.75
- decay_param: float32 [1024], P('tp'), may hold values from 5 to 8.5
- channel_gain: float32 [1024], replicated, may hold values from 0.1 to 1.9
- out_proj: float32 [1024, 2048], P('fs', 'tp'), may hold values from -0.1875 to 0.1875
- post_gain: float32 [2048], replicated, may hold values from 0.1 to 1.9
- post_gate: float32 [2048, 2816], P('fs', 'tp'), may hold values from -0.125 to 0.125
- post_up: float32 [2048, 2816], P('fs', 'tp'), may hold values from -0.125 to 0.125
- post_down: float32 [2816, 2048], P('fs', 'tp'), may hold values from -0.109375 to 0.109375
Outputs:
- layer_out: bfloat16 [4096, 2048], P('fs', 'tp')
The draws below stay inside these ranges and needn't reach their ends.
All inputs are finite; a program needn't handle non-finite values.
Results may differ from the reference program's by a relative error of at most 0.012.
Values may be sent and summed in bfloat16 or wider, within the bound.
A program may use at most 64 MiB of HBM per device.

```python
import jax
import jax.numpy as jnp
from jax import lax

D = 2048
FF = 2816
HEADS = 16
BLOCK = 64
CONV = 4
SEQ_LEN = 128
DL = 1024
TOKENS = 4096


def block_levels(key, dims, shards, least, largest):
    factor_of = 1.0
    for dim, blocks in shards:
        draws = jax.random.uniform(jax.random.fold_in(jax.random.fold_in(key, 6), dim), (blocks,), jnp.float32, least / len(shards), largest / len(shards))
        factor_of = factor_of * jnp.repeat(jnp.exp(draws), dims[dim] // blocks).reshape((-1,) + (1,) * (len(dims) - 1 - dim))
    return factor_of


def noise(key, shape, scale, bound, cuts=(), held_as=jnp.bfloat16):
    level = block_levels(key, shape, cuts, -0.22, 0.18) if cuts else 1.0
    result = jax.random.normal(key, shape, jnp.float32) * scale * level
    return jnp.minimum(jnp.maximum(result, -bound), bound).astype(held_as)


def setup_inputs(seed: int = 0) -> dict:
    streams_of = jax.random.split(jax.random.key(seed), 19)
    return {
        "tokens": noise(streams_of[0], (TOKENS, D), 1.0, 6.0, ((0, 8), (1, 4))),
        "pre_gain": jnp.clip(1.0 + 0.18 * jax.random.normal(streams_of[1], (D,), jnp.float32), 0.1, 1.9),
        "pre_gate": noise(streams_of[2], (D, FF), D ** -0.5, 0.125, ((0, 8), (1, 4)), jnp.float32),
        "pre_up": noise(streams_of[3], (D, FF), D ** -0.5, 0.125, ((0, 8), (1, 4)), jnp.float32),
        "pre_down": noise(streams_of[4], (FF, D), FF ** -0.5, 0.109375, ((0, 8), (1, 4)), jnp.float32),
        "mix_gain": jnp.clip(1.0 + 0.18 * jax.random.normal(streams_of[5], (D,), jnp.float32), 0.1, 1.9),
        "branch_proj": noise(streams_of[6], (D, DL), D ** -0.5, 0.125, ((0, 8), (1, 4)), jnp.float32),
        "gate_proj": noise(streams_of[7], (D, DL), D ** -0.5, 0.125, ((0, 8), (1, 4)), jnp.float32),
        "conv_taps": noise(streams_of[8], (CONV, DL), CONV ** -0.5, 3.0, ((1, 4),), jnp.float32),
        "retain_blocks": noise(streams_of[9], (HEADS, BLOCK, BLOCK), BLOCK ** -0.5, 0.75, ((0, 4),), jnp.float32),
        "admit_blocks": noise(streams_of[10], (HEADS, BLOCK, BLOCK), BLOCK ** -0.5, 0.75, ((0, 4),), jnp.float32),
        "decay_param": jnp.clip(5.0 + 3.5 * jax.random.uniform(streams_of[11], (DL,), jnp.float32) ** block_levels(streams_of[11], (DL,), ((0, 4),), -0.2, 0.2), 5.0, 8.5),
        "channel_gain": jnp.clip(1.0 + 0.18 * jax.random.normal(streams_of[12], (DL,), jnp.float32), 0.1, 1.9),
        "out_proj": noise(streams_of[13], (DL, D), DL ** -0.5, 0.1875, ((0, 8), (1, 4)), jnp.float32),
        "post_gain": jnp.clip(1.0 + 0.18 * jax.random.normal(streams_of[14], (D,), jnp.float32), 0.1, 1.9),
        "post_gate": noise(streams_of[15], (D, FF), D ** -0.5, 0.125, ((0, 8), (1, 4)), jnp.float32),
        "post_up": noise(streams_of[16], (D, FF), D ** -0.5, 0.125, ((0, 8), (1, 4)), jnp.float32),
        "post_down": noise(streams_of[17], (FF, D), FF ** -0.5, 0.109375, ((0, 8), (1, 4)), jnp.float32),
    }


EPSILON = 1e-06
DECAY_SCALE = 8.0

def normalize(values, norm_gain):
    floats = values.astype(jnp.float32)
    scaled = floats * lax.rsqrt(lax.optimization_barrier(jnp.mean(floats * floats, axis=-1, keepdims=True)) + EPSILON)
    return (scaled * norm_gain).astype(jnp.bfloat16)

def product(operand, matrix):
    return jnp.dot(operand, matrix.astype(jnp.bfloat16), preferred_element_type=jnp.float32)

def combine(earlier, latter):
    keep_early, add_early = earlier
    keep_late, add_late = latter
    return (keep_early * keep_late, keep_late * add_early + add_late)

def feed_forward(residual, norm_gain, gate_matrix, up_matrix, down_matrix):
    normed = normalize(residual, norm_gain)
    hidden = (jax.nn.silu(product(normed, gate_matrix)) * product(normed, up_matrix)).astype(jnp.bfloat16)
    return (residual.astype(jnp.float32) + 0.5 * product(hidden, down_matrix)).astype(jnp.bfloat16)

def block_gate(convolved, blocks):
    rounded = lax.optimization_barrier(blocks.astype(jnp.bfloat16)).astype(jnp.float32)
    grouped = convolved.astype(jnp.float32).reshape(convolved.shape[0], convolved.shape[1], blocks.shape[0], blocks.shape[1])
    mixed = jnp.einsum('sthi,hij->sthj', grouped, rounded)
    return jax.nn.sigmoid(mixed).reshape(convolved.shape)

def recurrent_mixer(residual, norm_gain, branch_matrix, gate_matrix, conv_taps, retain_blocks, admit_blocks, decay_param, channel_gain, out_matrix):
    normed = normalize(residual, norm_gain)
    branch = product(normed, branch_matrix)
    gate_act = product(normed, gate_matrix)
    sequences = residual.shape[0] // SEQ_LEN
    channel_count = branch.shape[1]
    framed = branch.reshape(sequences, SEQ_LEN, channel_count)
    padded = jnp.pad(framed, ((0, 0), (CONV - 1, 0), (0, 0)))
    convolved = jnp.zeros_like(framed)
    for tap_index in range(CONV):
        convolved = convolved + padded[:, tap_index:tap_index + SEQ_LEN] * conv_taps[tap_index]
    convolved = convolved.astype(jnp.bfloat16)
    retained = block_gate(convolved, retain_blocks)
    admitted = block_gate(convolved, admit_blocks)
    log_keep = -DECAY_SCALE * retained * jax.nn.softplus(-decay_param)
    inject = jnp.sqrt(-jnp.expm1(2.0 * log_keep)) * admitted * convolved.astype(jnp.float32)
    _, states = lax.associative_scan(combine, (jnp.exp(log_keep), inject), axis=1)
    mixed_rows = (states.reshape(residual.shape[0], channel_count) * jax.nn.gelu(gate_act)).astype(jnp.bfloat16)
    mixed_normed = normalize(mixed_rows, channel_gain)
    return (residual.astype(jnp.float32) + product(mixed_normed, out_matrix)).astype(jnp.bfloat16)

def reference(tokens, pre_gain, pre_gate, pre_up, pre_down, mix_gain, branch_proj, gate_proj, conv_taps, retain_blocks, admit_blocks, decay_param, channel_gain, out_proj, post_gain, post_gate, post_up, post_down):
    after_pre = feed_forward(tokens, pre_gain, pre_gate, pre_up, pre_down)
    after_mix = recurrent_mixer(after_pre, mix_gain, branch_proj, gate_proj, conv_taps, retain_blocks, admit_blocks, decay_param, channel_gain, out_proj)
    return feed_forward(after_mix, post_gain, post_gate, post_up, post_down)
```

```python
import jax
import jax.numpy as jnp
from jax import lax
from jax.experimental import pallas as pl
from jax.experimental.pallas import tpu as pltpu
from jax.sharding import PartitionSpec as P

SEQ_LEN = 128


EPSILON = 1e-06
DECAY_SCALE = 8.0


def normalize(values, norm_gain):
    floats = values.astype(jnp.float32)
    scaled = floats * lax.rsqrt(jnp.mean(floats * floats, axis=-1, keepdims=True) + EPSILON)
    return (scaled * norm_gain).astype(jnp.bfloat16)


def widen(residual):
    return lax.all_gather(residual, "tp", axis=1, tiled=True)


def contract(operand, stacked):
    return jnp.dot(
        operand,
        lax.all_gather(stacked.astype(jnp.bfloat16), "fs", axis=0, tiled=True),
        preferred_element_type=jnp.float32,
    )


def feed_forward(residual, norm_gain, gate_matrix, up_matrix, down_matrix):
    normed = normalize(widen(residual), norm_gain)
    products = contract(normed, jnp.concatenate((gate_matrix, up_matrix), axis=1))
    split_at = gate_matrix.shape[1]
    hidden = (jax.nn.silu(products[:, :split_at]) * products[:, split_at:]).astype(jnp.bfloat16)
    all_hidden = lax.all_gather(hidden, "tp", axis=1, tiled=True)
    return (residual.astype(jnp.float32) + 0.5 * contract(all_hidden, down_matrix)).astype(
        jnp.bfloat16
    )


def shifted(values, distance, fill):
    row = lax.broadcasted_iota(jnp.int32, values.shape, 0)
    return jnp.where(row >= distance, pltpu.roll(values, distance, 0), fill)


def mix_sequence(branch, gate_act, taps, gates, sharpness):
    width = branch.shape[1]
    count = taps.shape[0]
    convolved = branch * taps[count - 1 : count]
    for back in range(1, count):
        convolved = convolved + shifted(branch, back, 0.0) * taps[count - 1 - back : count - back]
    convolved = convolved.astype(jnp.bfloat16)
    both = jax.nn.sigmoid(jnp.dot(convolved, gates, preferred_element_type=jnp.float32))
    log_keep = -DECAY_SCALE * both[:, :width] * sharpness
    keep = jnp.exp(log_keep)
    inject = (
        jnp.sqrt(jnp.tanh(-log_keep) * (1.0 + keep * keep))
        * both[:, width:]
        * convolved.astype(jnp.float32)
    )
    distance = 1
    while distance < branch.shape[0]:
        inject = keep * shifted(inject, distance, 0.0) + inject
        keep = keep * shifted(keep, distance, 1.0)
        distance *= 2
    return (inject * jax.nn.gelu(gate_act)).astype(jnp.bfloat16)


def mix_kernel(products_ref, taps_ref, gates_ref, sharp_ref, out_ref):
    width = out_ref.shape[1]
    out_ref[...] = mix_sequence(
        products_ref[:, :width],
        products_ref[:, width:],
        taps_ref[...],
        gates_ref[...],
        sharp_ref[...],
    )


def spread_blocks(blocks):
    count, size, _ = blocks.shape
    eye = jnp.eye(count, dtype=blocks.dtype)
    wide = eye[:, None, :, None] * blocks[:, :, None, :]
    return wide.reshape(count * size, count * size).astype(jnp.bfloat16)


def recurrent_mixer(
    residual,
    norm_gain,
    branch_matrix,
    gate_matrix,
    conv_taps,
    retain_blocks,
    admit_blocks,
    decay_param,
    channel_gain,
    out_matrix,
):
    normed = normalize(widen(residual), norm_gain)
    products = contract(normed, jnp.concatenate((branch_matrix, gate_matrix), axis=1))
    width = branch_matrix.shape[1]
    rows = residual.shape[0]
    gates = jnp.concatenate((spread_blocks(retain_blocks), spread_blocks(admit_blocks)), axis=1)
    sharpness = jax.nn.softplus(-decay_param)[None, :]
    whole = lambda array: pl.BlockSpec(array.shape, lambda i: (0, 0))
    mixed_rows = pl.pallas_call(
        mix_kernel,
        grid=(rows // SEQ_LEN,),
        in_specs=[
            pl.BlockSpec((SEQ_LEN, 2 * width), lambda i: (i, 0)),
            whole(conv_taps),
            whole(gates),
            whole(sharpness),
        ],
        out_specs=pl.BlockSpec((SEQ_LEN, width), lambda i: (i, 0)),
        out_shape=jax.ShapeDtypeStruct((rows, width), jnp.bfloat16),
        cost_estimate=pl.CostEstimate(
            flops=rows * width * 1200, bytes_accessed=rows * width * 10, transcendentals=0
        ),
    )(products, conv_taps, gates, sharpness)
    all_channels = lax.all_gather(mixed_rows, "tp", axis=1, tiled=True)
    mixed_normed = normalize(all_channels, channel_gain)
    return (residual.astype(jnp.float32) + contract(mixed_normed, out_matrix)).astype(jnp.bfloat16)


def local(
    tokens,
    pre_gain,
    pre_gate,
    pre_up,
    pre_down,
    mix_gain,
    branch_proj,
    gate_proj,
    conv_taps,
    retain_blocks,
    admit_blocks,
    decay_param,
    channel_gain,
    out_proj,
    post_gain,
    post_gate,
    post_up,
    post_down,
):
    after_pre = feed_forward(tokens, pre_gain, pre_gate, pre_up, pre_down)
    after_mix = recurrent_mixer(
        after_pre,
        mix_gain,
        branch_proj,
        gate_proj,
        conv_taps,
        retain_blocks,
        admit_blocks,
        decay_param,
        channel_gain,
        out_proj,
    )
    return feed_forward(after_mix, post_gain, post_gate, post_up, post_down)


def solution(mesh):
    placed = (
        P("fs", "tp"),
        P(),
        P("fs", "tp"),
        P("fs", "tp"),
        P("fs", "tp"),
        P(),
        P("fs", "tp"),
        P("fs", "tp"),
        P(None, "tp"),
        P("tp", None, None),
        P("tp", None, None),
        P("tp"),
        P(),
        P("fs", "tp"),
        P(),
        P("fs", "tp"),
        P("fs", "tp"),
        P("fs", "tp"),
    )
    return jax.shard_map(
        local, mesh=mesh, in_specs=placed, out_specs=P("fs", "tp"), check_vma=False
    )
```

```python
import functools

import jax
import jax.numpy as jnp
from jax import lax
from jax.experimental import pallas as pl
from jax.experimental.pallas import tpu as pltpu
from jax.sharding import PartitionSpec as P

SEQ_LEN = 128


EPSILON = 1e-06
DECAY_SCALE = 8.0


def normalize(values, norm_gain):
    floats = values.astype(jnp.float32)
    scaled = floats * lax.rsqrt(jnp.mean(floats * floats, axis=-1, keepdims=True) + EPSILON)
    return (scaled * norm_gain).astype(jnp.bfloat16)


def widen(residual):
    return lax.all_gather(residual, "tp", axis=1, tiled=True)


def contract(operand, stacked):
    return jnp.dot(
        operand,
        lax.all_gather(stacked.astype(jnp.bfloat16), "fs", axis=0, tiled=True),
        preferred_element_type=jnp.float32,
    )


def feed_forward(residual, norm_gain, gate_matrix, up_matrix, down_matrix):
    normed = normalize(widen(residual), norm_gain)
    products = contract(normed, jnp.concatenate((gate_matrix, up_matrix), axis=1))
    split_at = gate_matrix.shape[1]
    hidden = (jax.nn.silu(products[:, :split_at]) * products[:, split_at:]).astype(jnp.bfloat16)
    all_hidden = lax.all_gather(hidden, "tp", axis=1, tiled=True)
    return (residual.astype(jnp.float32) + 0.5 * contract(all_hidden, down_matrix)).astype(
        jnp.bfloat16
    )


def shifted(values, distance, fill):
    row = lax.broadcasted_iota(jnp.int32, values.shape, 0)
    return jnp.where(row >= distance, pltpu.roll(values, distance, 0), fill)


def mix_sequence(branch, gate_act, taps, gates, sharpness):
    width = branch.shape[1]
    count = taps.shape[0]
    convolved = branch * taps[count - 1 : count]
    for back in range(1, count):
        convolved = convolved + shifted(branch, back, 0.0) * taps[count - 1 - back : count - back]
    convolved = convolved.astype(jnp.bfloat16)
    both = jax.nn.sigmoid(jnp.dot(convolved, gates, preferred_element_type=jnp.float32))
    log_keep = -DECAY_SCALE * both[:, :width] * sharpness
    keep = jnp.exp(log_keep)
    inject = (
        jnp.sqrt(jnp.tanh(-log_keep) * (1.0 + keep * keep))
        * both[:, width:]
        * convolved.astype(jnp.float32)
    )
    distance = 1
    while distance < branch.shape[0]:
        inject = keep * shifted(inject, distance, 0.0) + inject
        keep = keep * shifted(keep, distance, 1.0)
        distance *= 2
    return (inject * jax.nn.gelu(gate_act)).astype(jnp.bfloat16)


def mix_kernel(products_ref, taps_ref, gates_ref, sharp_ref, out_ref):
    width = out_ref.shape[1]
    out_ref[...] = mix_sequence(
        products_ref[:, :width],
        products_ref[:, width:],
        taps_ref[...],
        gates_ref[...],
        sharp_ref[...],
    )


def spread_blocks(blocks):
    count, size, _ = blocks.shape
    eye = jnp.eye(count, dtype=blocks.dtype)
    wide = eye[:, None, :, None] * blocks[:, :, None, :]
    return wide.reshape(count * size, count * size).astype(jnp.bfloat16)


def recurrent_mixer(
    residual,
    norm_gain,
    branch_matrix,
    gate_matrix,
    conv_taps,
    retain_blocks,
    admit_blocks,
    decay_param,
    channel_gain,
    out_matrix,
):
    normed = normalize(widen(residual), norm_gain)
    products = contract(normed, jnp.concatenate((branch_matrix, gate_matrix), axis=1))
    width = branch_matrix.shape[1]
    rows = residual.shape[0]
    gates = jnp.concatenate((spread_blocks(retain_blocks), spread_blocks(admit_blocks)), axis=1)
    sharpness = jax.nn.softplus(-decay_param)[None, :]
    whole = lambda array: pl.BlockSpec(array.shape, lambda i: (0, 0))
    mixed_rows = pl.pallas_call(
        mix_kernel,
        grid=(rows // SEQ_LEN,),
        in_specs=[
            pl.BlockSpec((SEQ_LEN, 2 * width), lambda i: (i, 0)),
            whole(conv_taps),
            whole(gates),
            whole(sharpness),
        ],
        out_specs=pl.BlockSpec((SEQ_LEN, width), lambda i: (i, 0)),
        out_shape=jax.ShapeDtypeStruct((rows, width), jnp.bfloat16),
        cost_estimate=pl.CostEstimate(
            flops=rows * width * 1200, bytes_accessed=rows * width * 10, transcendentals=0
        ),
    )(products, conv_taps, gates, sharpness)
    all_channels = lax.all_gather(mixed_rows, "tp", axis=1, tiled=True)
    mixed_normed = normalize(all_channels, channel_gain)
    return (residual.astype(jnp.float32) + contract(mixed_normed, out_matrix)).astype(jnp.bfloat16)


ROW_TILE = 256
MESH = pl.DeviceIdType.MESH


class Exchange:
    def __init__(self):
        self.sent = []

    def send(self, source, target, send_sem, recv_sem, device, condition=None):
        copy = pltpu.make_async_remote_copy(
            src_ref=source,
            dst_ref=target,
            send_sem=send_sem,
            recv_sem=recv_sem,
            device_id=device,
            device_id_type=MESH,
        )
        when(condition, copy.start)
        self.sent.append((copy, condition))

    def drain(self):
        for copy, condition in self.sent:
            when(condition, copy.wait_send)


def when(condition, action):
    if condition is None:
        action()
    else:
        pl.when(condition)(action)


def layer_kernel(fs_size, tp_size, *refs):
    (tokens, pre_gain, mix_gain, channel_gain, post_gain, taps, gates, sharpness) = refs[:8]
    shards = refs[8:16]
    out = refs[16]
    whole = refs[17:25]
    first, second, third, hidden_one, hidden_two, channels, normed = refs[25:32]
    recv_sem, line_sem, back_sem, pair_sem, keep_sem = refs[32:37]
    tp_recv, tp_peer, tp_own, tp_pass, token_sem = refs[37:42]

    f = lax.axis_index("fs")
    t = lax.axis_index("tp")
    x = lax.rem(f, 2)
    z = f // 2
    depth = fs_size // 2
    half = tp_size // 2
    across = {"fs": f + 1 - 2 * x}
    above = {"fs": lax.rem(f + 2, fs_size)}
    below = {"fs": lax.rem(f + fs_size - 2, fs_size)}
    has_above = z < depth - 1
    has_below = z > 0
    twin = t + 1 - 2 * lax.rem(t, 2)
    peers = [lax.rem(t + 2 * k, tp_size) for k in range(1, half)]
    links = Exchange()

    barrier = pltpu.get_barrier_semaphore()
    greeted = [(across, None), (above, has_above), (below, has_below), ({"tp": twin}, None)]
    greeted += [({"tp": peer}, None) for peer in peers]
    for device, condition in greeted:
        when(
            condition,
            functools.partial(
                pl.semaphore_signal, barrier, inc=1, device_id=device, device_id_type=MESH
            ),
        )
    line_ends = (z == 0).astype(jnp.int32) + (z == depth - 1).astype(jnp.int32)
    pl.semaphore_wait(barrier, len(greeted) - line_ends)

    def shard_at(p, owner):
        rows = shards[p].shape[0]
        return whole[p].at[pl.ds(pl.multiple_of(owner * rows, rows), rows)]

    def arrive(p, owner, condition=None):
        place = shard_at(p, owner)
        copy = pltpu.make_async_remote_copy(
            src_ref=place,
            dst_ref=place,
            send_sem=pair_sem.at[p, 0],
            recv_sem=recv_sem.at[p, owner],
            device_id=across,
            device_id_type=MESH,
        )
        when(condition, copy.wait_recv)

    def own_copy(p):
        return pltpu.make_async_copy(shards[p], shard_at(p, f), keep_sem.at[p])

    def launch(p):
        place, sem = shard_at(p, f), recv_sem.at[p, f]
        links.send(shards[p], place, line_sem.at[p, f], sem, above, has_above)
        links.send(shards[p], place, back_sem.at[p, 0], sem, below, has_below)
        links.send(shards[p], place, pair_sem.at[p, z], sem, across)
        own_copy(p).start()

    def launch_pair(p):
        owner = f + 1 - 2 * x
        arrive(p, owner)
        place, sem = shard_at(p, owner), recv_sem.at[p, owner]
        links.send(place, place, line_sem.at[p, owner], sem, above, has_above)
        links.send(place, place, back_sem.at[p, 1], sem, below, has_below)

    def relay(p, distance, column, cross):
        for sign, edge, there in ((-1, above, has_above), (1, below, has_below)):
            level = z + sign * distance
            exists = (level >= 0) & (level < depth)
            level = lax.rem(level + depth, depth)
            owner = level * 2 + column
            arrive(p, owner, exists)
            place, sem = shard_at(p, owner), recv_sem.at[p, owner]
            links.send(place, place, line_sem.at[p, owner], sem, edge, exists & there)
            if cross:
                links.send(place, place, pair_sem.at[p, level], sem, across, exists)

    count = len(shards)
    direct = (2,)

    def step(number):
        for p in range(count):
            if max(p - 1, 0) == number:
                launch(p)
        for p in range(count):
            if p in direct:
                if p + 1 == number:
                    launch_pair(p)
                if 1 <= number - p - 1 < depth:
                    relay(p, number - p - 1, 1 - x, False)
            if 1 <= number - p < depth:
                relay(p, number - p, x, p not in direct)

    def ready(p):
        own_copy(p).wait()
        if p not in direct:
            for level in range(depth):
                arrive(p, level * 2 + 1 - x)

    def spread(array, index):
        for k, peer in enumerate(peers):
            links.send(
                array.at[t], array.at[t], tp_peer.at[index, k], tp_recv.at[index, t], {"tp": peer}
            )
        links.send(
            array.at[t], array.at[t], tp_own.at[index], tp_recv.at[index, t], {"tp": twin}
        )

    def landed(array, index, slot):
        pltpu.make_async_remote_copy(
            src_ref=array.at[slot],
            dst_ref=array.at[slot],
            send_sem=tp_own.at[index],
            recv_sem=tp_recv.at[index, slot],
            device_id={"tp": twin},
            device_id_type=MESH,
        ).wait_recv()

    def collect(array, index):
        for k, peer in enumerate(peers):
            landed(array, index, peer)
            links.send(
                array.at[peer],
                array.at[peer],
                tp_pass.at[index, k],
                tp_recv.at[index, peer],
                {"tp": twin},
            )
        landed(array, index, twin)
        for k in range(1, half):
            landed(array, index, lax.rem(twin + 2 * k, tp_size))

    total_rows = tokens.shape[0]

    def tiles(size, body):
        def run(i, carry):
            body(pl.ds(pl.multiple_of(i * size, size), size))
            return carry

        lax.fori_loop(0, total_rows // size, run, 0)

    def norm_slots(array, gain):
        width = array.shape[2]
        features = width * tp_size

        def body(rows):
            parts = [array[s, rows, :].astype(jnp.float32) for s in range(tp_size)]
            squares = sum(jnp.sum(part * part, axis=-1, keepdims=True) for part in parts)
            scale = lax.rsqrt(squares / features + EPSILON)
            for s, part in enumerate(parts):
                at = slice(s * width, (s + 1) * width)
                normed[rows, at] = (part * scale * gain[:, at]).astype(jnp.bfloat16)

        tiles(64, body)

    def dot(left, right):
        return jnp.dot(left, right, preferred_element_type=jnp.float32)

    def gated(gate, up, hidden):
        def body(rows):
            values = normed[rows, :]
            product = jax.nn.silu(dot(values, gate[...])) * dot(values, up[...])
            hidden[t, rows, :] = product.astype(jnp.bfloat16)

        tiles(ROW_TILE, body)

    def lower(hidden, down, residual, store):
        width = hidden.shape[2]

        def body(rows):
            total = sum(
                dot(hidden[s, rows, :], down[s * width : (s + 1) * width, :])
                for s in range(tp_size)
            )
            value = residual[t, rows, :].astype(jnp.float32) + 0.5 * total
            store(rows, value.astype(jnp.bfloat16))

        tiles(ROW_TILE, body)

    def mix(rows):
        width = channels.shape[2]
        products = dot(normed[rows, :], whole[3][...])
        channels[t, rows, :] = mix_sequence(
            products[:, :width], products[:, width:], taps[...], gates[...], sharpness[...]
        )

    def put(array):
        def store(rows, value):
            array[t, rows, :] = value

        return store

    def finish(rows, value):
        out[rows, :] = value

    def project(rows):
        width = channels.shape[2] * tp_size
        total = dot(normed[rows, :width], whole[4][...])
        third[t, rows, :] = (second[t, rows, :].astype(jnp.float32) + total).astype(jnp.bfloat16)

    local_tokens = pltpu.make_async_copy(tokens, first.at[t], token_sem)
    local_tokens.start()
    step(0)
    local_tokens.wait()
    spread(first, 0)
    step(1)
    step(2)
    collect(first, 0)
    norm_slots(first, pre_gain)
    step(3)
    step(4)
    step(5)
    ready(0)
    ready(1)
    gated(whole[0], whole[1], hidden_one)
    spread(hidden_one, 1)
    step(6)
    collect(hidden_one, 1)
    ready(2)
    lower(hidden_one, whole[2], first, put(second))
    spread(second, 2)
    step(7)
    collect(second, 2)
    norm_slots(second, mix_gain)
    ready(3)
    tiles(SEQ_LEN, mix)
    spread(channels, 3)
    step(8)
    collect(channels, 3)
    norm_slots(channels, channel_gain)
    ready(4)
    tiles(ROW_TILE, project)
    spread(third, 4)
    step(9)
    collect(third, 4)
    norm_slots(third, post_gain)
    for number in range(10, count + depth):
        step(number)
    ready(5)
    ready(6)
    gated(whole[5], whole[6], hidden_two)
    spread(hidden_two, 5)
    collect(hidden_two, 5)
    ready(7)
    lower(hidden_two, whole[7], third, finish)
    links.drain()


def fused(
    fs_size,
    tp_size,
    tokens,
    pre_gain,
    pre_gate,
    pre_up,
    pre_down,
    mix_gain,
    branch_proj,
    gate_proj,
    conv_taps,
    retain_blocks,
    admit_blocks,
    decay_param,
    channel_gain,
    out_proj,
    post_gain,
    post_gate,
    post_up,
    post_down,
):
    half_type = lambda array: array.astype(jnp.bfloat16)
    shards = [
        half_type(pre_gate),
        half_type(pre_up),
        half_type(pre_down),
        jnp.concatenate((half_type(branch_proj), half_type(gate_proj)), axis=1),
        half_type(out_proj),
        half_type(post_gate),
        half_type(post_up),
        half_type(post_down),
    ]
    gates = jnp.concatenate((spread_blocks(retain_blocks), spread_blocks(admit_blocks)), axis=1)
    sharpness = jax.nn.softplus(-decay_param)[None, :]
    rows, width = tokens.shape
    hidden = pre_gate.shape[1]
    operands = [
        tokens,
        pre_gain[None],
        mix_gain[None],
        channel_gain[None],
        post_gain[None],
        conv_taps,
        gates,
        sharpness,
        *shards,
    ]
    dma = pltpu.SemaphoreType.DMA
    count = len(shards)
    stacked = lambda columns: pltpu.VMEM((tp_size, rows, columns), jnp.bfloat16)
    peers = max(tp_size // 2 - 1, 1)
    return pl.pallas_call(
        functools.partial(layer_kernel, fs_size, tp_size),
        out_shape=jax.ShapeDtypeStruct(tokens.shape, tokens.dtype),
        in_specs=[pl.BlockSpec(memory_space=pltpu.VMEM)] * len(operands),
        out_specs=pl.BlockSpec(memory_space=pltpu.VMEM),
        scratch_shapes=[
            *(pltpu.VMEM((fs_size * s.shape[0], s.shape[1]), jnp.bfloat16) for s in shards),
            stacked(width),
            stacked(width),
            stacked(width),
            stacked(hidden),
            stacked(hidden),
            stacked(branch_proj.shape[1]),
            pltpu.VMEM((rows, width * tp_size), jnp.bfloat16),
            dma((count, fs_size)),
            dma((count, fs_size)),
            dma((count, 2)),
            dma((count, fs_size // 2)),
            dma((count,)),
            dma((6, tp_size)),
            dma((6, peers)),
            dma((6,)),
            dma((6, peers)),
            dma,
        ],
        compiler_params=pltpu.CompilerParams(
            collective_id=0, has_side_effects=True, vmem_limit_bytes=62 * 2**20
        ),
    )(*operands)


def fits_fused(fs_size, tp_size, arrays):
    shards = [a for i, a in enumerate(arrays) if i in (2, 3, 4, 6, 7, 13, 15, 16, 17)]
    rows_fit = all(a.shape[0] % 16 == 0 for a in shards)
    lanes_fit = all(arrays[i].shape[1] % 128 == 0 for i in (0, 6, 7))
    tiles_fit = arrays[0].shape[0] % ROW_TILE == 0 and arrays[2].shape[1] % 16 == 0
    return (
        rows_fit
        and lanes_fit
        and tiles_fit
        and fs_size % 2 == 0
        and 4 <= fs_size <= 16
        and tp_size % 2 == 0
    )


def local(
    tokens,
    pre_gain,
    pre_gate,
    pre_up,
    pre_down,
    mix_gain,
    branch_proj,
    gate_proj,
    conv_taps,
    retain_blocks,
    admit_blocks,
    decay_param,
    channel_gain,
    out_proj,
    post_gain,
    post_gate,
    post_up,
    post_down,
):
    after_pre = feed_forward(tokens, pre_gain, pre_gate, pre_up, pre_down)
    after_mix = recurrent_mixer(
        after_pre,
        mix_gain,
        branch_proj,
        gate_proj,
        conv_taps,
        retain_blocks,
        admit_blocks,
        decay_param,
        channel_gain,
        out_proj,
    )
    return feed_forward(after_mix, post_gain, post_gate, post_up, post_down)


def solution(mesh):
    placed = (
        P("fs", "tp"),
        P(),
        P("fs", "tp"),
        P("fs", "tp"),
        P("fs", "tp"),
        P(),
        P("fs", "tp"),
        P("fs", "tp"),
        P(None, "tp"),
        P("tp", None, None),
        P("tp", None, None),
        P("tp"),
        P(),
        P("fs", "tp"),
        P(),
        P("fs", "tp"),
        P("fs", "tp"),
        P("fs", "tp"),
    )
    fs_size, tp_size = mesh.shape["fs"], mesh.shape["tp"]

    def layer(*arrays):
        if fits_fused(fs_size, tp_size, arrays):
            return fused(fs_size, tp_size, *arrays)
        return local(*arrays)

    return jax.shard_map(
        layer, mesh=mesh, in_specs=placed, out_specs=P("fs", "tp"), check_vma=False
    )
```

```python
import functools

import jax
import jax.numpy as jnp
from jax import lax
from jax.experimental import pallas as pl
from jax.experimental.pallas import tpu as pltpu
from jax.sharding import PartitionSpec as P

SEQ_LEN = 128


EPSILON = 1e-06
DECAY_SCALE = 8.0


def normalize(values, norm_gain):
    floats = values.astype(jnp.float32)
    scaled = floats * lax.rsqrt(jnp.mean(floats * floats, axis=-1, keepdims=True) + EPSILON)
    return (scaled * norm_gain).astype(jnp.bfloat16)


def widen(residual):
    return lax.all_gather(residual, "tp", axis=1, tiled=True)


def contract(operand, stacked):
    return jnp.dot(
        operand,
        lax.all_gather(stacked.astype(jnp.bfloat16), "fs", axis=0, tiled=True),
        preferred_element_type=jnp.float32,
    )


def feed_forward(residual, norm_gain, gate_matrix, up_matrix, down_matrix):
    normed = normalize(widen(residual), norm_gain)
    products = contract(normed, jnp.concatenate((gate_matrix, up_matrix), axis=1))
    split_at = gate_matrix.shape[1]
    hidden = (jax.nn.silu(products[:, :split_at]) * products[:, split_at:]).astype(jnp.bfloat16)
    all_hidden = lax.all_gather(hidden, "tp", axis=1, tiled=True)
    return (residual.astype(jnp.float32) + 0.5 * contract(all_hidden, down_matrix)).astype(
        jnp.bfloat16
    )


def shifted(values, distance, fill):
    row = lax.broadcasted_iota(jnp.int32, values.shape, 0)
    return jnp.where(row >= distance, pltpu.roll(values, distance, 0), fill)


def mix_sequence(branch, gate_act, taps, gates, sharpness):
    width = branch.shape[1]
    count = taps.shape[0]
    convolved = branch * taps[count - 1 : count]
    for back in range(1, count):
        convolved = convolved + shifted(branch, back, 0.0) * taps[count - 1 - back : count - back]
    convolved = convolved.astype(jnp.bfloat16)
    both = jax.nn.sigmoid(jnp.dot(convolved, gates, preferred_element_type=jnp.float32))
    log_keep = -DECAY_SCALE * both[:, :width] * sharpness
    keep = jnp.exp(log_keep)
    inject = (
        jnp.sqrt(jnp.tanh(-log_keep) * (1.0 + keep * keep))
        * both[:, width:]
        * convolved.astype(jnp.float32)
    )
    distance = 1
    while distance < branch.shape[0]:
        inject = keep * shifted(inject, distance, 0.0) + inject
        keep = keep * shifted(keep, distance, 1.0)
        distance *= 2
    return (inject * jax.nn.gelu(gate_act)).astype(jnp.bfloat16)


def mix_kernel(products_ref, taps_ref, gates_ref, sharp_ref, out_ref):
    width = out_ref.shape[1]
    out_ref[...] = mix_sequence(
        products_ref[:, :width],
        products_ref[:, width:],
        taps_ref[...],
        gates_ref[...],
        sharp_ref[...],
    )


def spread_blocks(blocks):
    count, size, _ = blocks.shape
    eye = jnp.eye(count, dtype=blocks.dtype)
    wide = eye[:, None, :, None] * blocks[:, :, None, :]
    return wide.reshape(count * size, count * size).astype(jnp.bfloat16)


def recurrent_mixer(
    residual,
    norm_gain,
    branch_matrix,
    gate_matrix,
    conv_taps,
    retain_blocks,
    admit_blocks,
    decay_param,
    channel_gain,
    out_matrix,
):
    normed = normalize(widen(residual), norm_gain)
    products = contract(normed, jnp.concatenate((branch_matrix, gate_matrix), axis=1))
    width = branch_matrix.shape[1]
    rows = residual.shape[0]
    gates = jnp.concatenate((spread_blocks(retain_blocks), spread_blocks(admit_blocks)), axis=1)
    sharpness = jax.nn.softplus(-decay_param)[None, :]
    whole = lambda array: pl.BlockSpec(array.shape, lambda i: (0, 0))
    mixed_rows = pl.pallas_call(
        mix_kernel,
        grid=(rows // SEQ_LEN,),
        in_specs=[
            pl.BlockSpec((SEQ_LEN, 2 * width), lambda i: (i, 0)),
            whole(conv_taps),
            whole(gates),
            whole(sharpness),
        ],
        out_specs=pl.BlockSpec((SEQ_LEN, width), lambda i: (i, 0)),
        out_shape=jax.ShapeDtypeStruct((rows, width), jnp.bfloat16),
        cost_estimate=pl.CostEstimate(
            flops=rows * width * 1200, bytes_accessed=rows * width * 10, transcendentals=0
        ),
    )(products, conv_taps, gates, sharpness)
    all_channels = lax.all_gather(mixed_rows, "tp", axis=1, tiled=True)
    mixed_normed = normalize(all_channels, channel_gain)
    return (residual.astype(jnp.float32) + contract(mixed_normed, out_matrix)).astype(jnp.bfloat16)


ROW_TILE = 256
MESH = pl.DeviceIdType.MESH


class Exchange:
    def __init__(self):
        self.sent = []

    def send(self, source, target, send_sem, recv_sem, device, condition=None):
        copy = pltpu.make_async_remote_copy(
            src_ref=source,
            dst_ref=target,
            send_sem=send_sem,
            recv_sem=recv_sem,
            device_id=device,
            device_id_type=MESH,
        )
        when(condition, copy.start)
        self.sent.append((copy, condition))

    def drain(self):
        for copy, condition in self.sent:
            when(condition, copy.wait_send)


def when(condition, action):
    if condition is None:
        action()
    else:
        pl.when(condition)(action)


def layer_kernel(fs_size, tp_size, *refs):
    (tokens, pre_gain, mix_gain, channel_gain, post_gain, taps, gates, sharpness) = refs[:8]
    shards = refs[8:16]
    out = refs[16]
    whole = refs[17:25]
    first, second, third, hidden_one, hidden_two, channels, normed = refs[25:32]
    recv_sem, line_sem, back_sem, pair_sem, keep_sem = refs[32:37]
    tp_recv, tp_peer, tp_own, tp_pass, token_sem = refs[37:42]

    f = lax.axis_index("fs")
    t = lax.axis_index("tp")
    x = lax.rem(f, 2)
    z = f // 2
    depth = fs_size // 2
    half = tp_size // 2
    across = {"fs": f + 1 - 2 * x}
    above = {"fs": lax.rem(f + 2, fs_size)}
    below = {"fs": lax.rem(f + fs_size - 2, fs_size)}
    has_above = z < depth - 1
    has_below = z > 0
    twin = t + 1 - 2 * lax.rem(t, 2)
    peers = [lax.rem(t + 2 * k, tp_size) for k in range(1, half)]
    links = Exchange()

    barrier = pltpu.get_barrier_semaphore()
    greeted = [(across, None), (above, has_above), (below, has_below), ({"tp": twin}, None)]
    greeted += [({"tp": peer}, None) for peer in peers]
    for device, condition in greeted:
        when(
            condition,
            functools.partial(
                pl.semaphore_signal, barrier, inc=1, device_id=device, device_id_type=MESH
            ),
        )
    line_ends = (z == 0).astype(jnp.int32) + (z == depth - 1).astype(jnp.int32)
    pl.semaphore_wait(barrier, len(greeted) - line_ends)

    def shard_at(p, owner):
        rows = shards[p].shape[0]
        return whole[p].at[pl.ds(pl.multiple_of(owner * rows, rows), rows)]

    def arrive(p, owner, condition=None):
        place = shard_at(p, owner)
        copy = pltpu.make_async_remote_copy(
            src_ref=place,
            dst_ref=place,
            send_sem=pair_sem.at[p, 0],
            recv_sem=recv_sem.at[p, owner],
            device_id=across,
            device_id_type=MESH,
        )
        when(condition, copy.wait_recv)

    def own_copy(p):
        return pltpu.make_async_copy(shards[p], shard_at(p, f), keep_sem.at[p])

    def launch(p):
        place, sem = shard_at(p, f), recv_sem.at[p, f]
        links.send(shards[p], place, line_sem.at[p, f], sem, above, has_above)
        links.send(shards[p], place, back_sem.at[p, 0], sem, below, has_below)
        links.send(shards[p], place, pair_sem.at[p, z], sem, across)
        own_copy(p).start()

    def launch_pair(p):
        owner = f + 1 - 2 * x
        arrive(p, owner)
        place, sem = shard_at(p, owner), recv_sem.at[p, owner]
        links.send(place, place, line_sem.at[p, owner], sem, above, has_above)
        links.send(place, place, back_sem.at[p, 1], sem, below, has_below)

    def relay(p, distance, column, cross):
        for sign, edge, there in ((-1, above, has_above), (1, below, has_below)):
            level = z + sign * distance
            exists = (level >= 0) & (level < depth)
            level = lax.rem(level + depth, depth)
            owner = level * 2 + column
            arrive(p, owner, exists)
            place, sem = shard_at(p, owner), recv_sem.at[p, owner]
            links.send(place, place, line_sem.at[p, owner], sem, edge, exists & there)
            if cross:
                links.send(place, place, pair_sem.at[p, level], sem, across, exists)

    count = len(shards)
    direct = (2,)

    def step(number):
        for p in range(count):
            if max(p - 1, 0) == number:
                launch(p)
        for p in range(count):
            if p in direct:
                if p + 1 == number:
                    launch_pair(p)
                if 1 <= number - p - 1 < depth:
                    relay(p, number - p - 1, 1 - x, False)
            if 1 <= number - p < depth:
                relay(p, number - p, x, p not in direct)

    def ready(p):
        own_copy(p).wait()
        if p not in direct:
            for level in range(depth):
                arrive(p, level * 2 + 1 - x)

    def spread(array, index):
        for k, peer in enumerate(peers):
            links.send(
                array.at[t], array.at[t], tp_peer.at[index, k], tp_recv.at[index, t], {"tp": peer}
            )
        links.send(
            array.at[t], array.at[t], tp_own.at[index], tp_recv.at[index, t], {"tp": twin}
        )

    def landed(array, index, slot):
        pltpu.make_async_remote_copy(
            src_ref=array.at[slot],
            dst_ref=array.at[slot],
            send_sem=tp_own.at[index],
            recv_sem=tp_recv.at[index, slot],
            device_id={"tp": twin},
            device_id_type=MESH,
        ).wait_recv()

    def collect(array, index):
        for k, peer in enumerate(peers):
            landed(array, index, peer)
            links.send(
                array.at[peer],
                array.at[peer],
                tp_pass.at[index, k],
                tp_recv.at[index, peer],
                {"tp": twin},
            )
        landed(array, index, twin)
        for k in range(1, half):
            landed(array, index, lax.rem(twin + 2 * k, tp_size))

    total_rows = tokens.shape[0]

    def tiles(size, body):
        def run(i, carry):
            body(pl.ds(pl.multiple_of(i * size, size), size))
            return carry

        lax.fori_loop(0, total_rows // size, run, 0)

    def norm_slots(array, gain):
        width = array.shape[2]
        features = width * tp_size

        def body(rows):
            parts = [array[s, rows, :].astype(jnp.float32) for s in range(tp_size)]
            squares = sum(jnp.sum(part * part, axis=-1, keepdims=True) for part in parts)
            scale = lax.rsqrt(squares / features + EPSILON)
            for s, part in enumerate(parts):
                at = slice(s * width, (s + 1) * width)
                normed[rows, at] = (part * scale * gain[:, at]).astype(jnp.bfloat16)

        tiles(64, body)

    def dot(left, right):
        return jnp.dot(left, right, preferred_element_type=jnp.float32)

    def gated(gate, up, hidden):
        features = gate.shape[1]
        width = hidden.shape[2]

        def turned(rows, matrix):
            return sum(
                lax.dot_general(
                    normed[rows, s * features : (s + 1) * features],
                    matrix[s * width : (s + 1) * width, :],
                    (((1,), (1,)), ((), ())),
                    preferred_element_type=jnp.float32,
                )
                for s in range(fs_size)
            )

        def body(rows):
            product = jax.nn.silu(turned(rows, gate)) * turned(rows, up)
            hidden[t, rows, :] = product.astype(jnp.bfloat16)

        tiles(ROW_TILE, body)

    def lower(hidden, down, residual, store):
        width = hidden.shape[2]

        def body(rows):
            total = sum(
                dot(hidden[s, rows, :], down[s * width : (s + 1) * width, :])
                for s in range(tp_size)
            )
            value = residual[t, rows, :].astype(jnp.float32) + 0.5 * total
            store(rows, value.astype(jnp.bfloat16))

        tiles(ROW_TILE, body)

    def mix(rows):
        width = channels.shape[2]
        products = dot(normed[rows, :], whole[3][...])
        channels[t, rows, :] = mix_sequence(
            products[:, :width], products[:, width:], taps[...], gates[...], sharpness[...]
        )

    def put(array):
        def store(rows, value):
            array[t, rows, :] = value

        return store

    def finish(rows, value):
        out[rows, :] = value

    def project(rows):
        width = channels.shape[2] * tp_size
        total = dot(normed[rows, :width], whole[4][...])
        third[t, rows, :] = (second[t, rows, :].astype(jnp.float32) + total).astype(jnp.bfloat16)

    local_tokens = pltpu.make_async_copy(tokens, first.at[t], token_sem)
    local_tokens.start()
    step(0)
    local_tokens.wait()
    spread(first, 0)
    step(1)
    step(2)
    collect(first, 0)
    norm_slots(first, pre_gain)
    step(3)
    step(4)
    step(5)
    ready(0)
    ready(1)
    gated(whole[0], whole[1], hidden_one)
    spread(hidden_one, 1)
    step(6)
    collect(hidden_one, 1)
    ready(2)
    lower(hidden_one, whole[2], first, put(second))
    spread(second, 2)
    step(7)
    collect(second, 2)
    norm_slots(second, mix_gain)
    ready(3)
    tiles(SEQ_LEN, mix)
    spread(channels, 3)
    step(8)
    collect(channels, 3)
    norm_slots(channels, channel_gain)
    ready(4)
    tiles(ROW_TILE, project)
    spread(third, 4)
    step(9)
    collect(third, 4)
    norm_slots(third, post_gain)
    for number in range(10, count + depth - 2):
        step(number)
    ready(5)
    ready(6)
    gated(whole[5], whole[6], hidden_two)
    spread(hidden_two, 5)
    for number in range(max(10, count + depth - 2), count + depth):
        step(number)
    collect(hidden_two, 5)
    ready(7)
    lower(hidden_two, whole[7], third, finish)
    links.drain()


def fused(
    fs_size,
    tp_size,
    tokens,
    pre_gain,
    pre_gate,
    pre_up,
    pre_down,
    mix_gain,
    branch_proj,
    gate_proj,
    conv_taps,
    retain_blocks,
    admit_blocks,
    decay_param,
    channel_gain,
    out_proj,
    post_gain,
    post_gate,
    post_up,
    post_down,
):
    half_type = lambda array: array.astype(jnp.bfloat16)
    shards = [
        half_type(pre_gate.T),
        half_type(pre_up.T),
        half_type(pre_down),
        jnp.concatenate((half_type(branch_proj), half_type(gate_proj)), axis=1),
        half_type(out_proj),
        half_type(post_gate.T),
        half_type(post_up.T),
        half_type(post_down),
    ]
    gates = jnp.concatenate((spread_blocks(retain_blocks), spread_blocks(admit_blocks)), axis=1)
    sharpness = jax.nn.softplus(-decay_param)[None, :]
    rows, width = tokens.shape
    hidden = pre_gate.shape[1]
    operands = [
        tokens,
        pre_gain[None],
        mix_gain[None],
        channel_gain[None],
        post_gain[None],
        conv_taps,
        gates,
        sharpness,
        *shards,
    ]
    dma = pltpu.SemaphoreType.DMA
    count = len(shards)
    stacked = lambda columns: pltpu.VMEM((tp_size, rows, columns), jnp.bfloat16)
    peers = max(tp_size // 2 - 1, 1)
    return pl.pallas_call(
        functools.partial(layer_kernel, fs_size, tp_size),
        out_shape=jax.ShapeDtypeStruct(tokens.shape, tokens.dtype),
        in_specs=[pl.BlockSpec(memory_space=pltpu.VMEM)] * len(operands),
        out_specs=pl.BlockSpec(memory_space=pltpu.VMEM),
        scratch_shapes=[
            *(pltpu.VMEM((fs_size * s.shape[0], s.shape[1]), jnp.bfloat16) for s in shards),
            stacked(width),
            stacked(width),
            stacked(width),
            stacked(hidden),
            stacked(hidden),
            stacked(branch_proj.shape[1]),
            pltpu.VMEM((rows, width * tp_size), jnp.bfloat16),
            dma((count, fs_size)),
            dma((count, fs_size)),
            dma((count, 2)),
            dma((count, fs_size // 2)),
            dma((count,)),
            dma((6, tp_size)),
            dma((6, peers)),
            dma((6,)),
            dma((6, peers)),
            dma,
        ],
        compiler_params=pltpu.CompilerParams(
            collective_id=0, has_side_effects=True, vmem_limit_bytes=62 * 2**20
        ),
    )(*operands)


def fits_fused(fs_size, tp_size, arrays):
    shards = [a for i, a in enumerate(arrays) if i in (2, 3, 4, 6, 7, 13, 15, 16, 17)]
    rows_fit = all(a.shape[0] % 16 == 0 for a in shards)
    lanes_fit = all(arrays[i].shape[1] % 128 == 0 for i in (0, 6, 7))
    tiles_fit = arrays[0].shape[0] % ROW_TILE == 0 and arrays[2].shape[1] % 16 == 0
    turned_fit = all(arrays[i].shape[0] % 128 == 0 for i in (2, 3, 15, 16))
    return (
        rows_fit
        and lanes_fit
        and tiles_fit
        and turned_fit
        and fs_size % 2 == 0
        and 4 <= fs_size <= 16
        and tp_size % 2 == 0
    )


def local(
    tokens,
    pre_gain,
    pre_gate,
    pre_up,
    pre_down,
    mix_gain,
    branch_proj,
    gate_proj,
    conv_taps,
    retain_blocks,
    admit_blocks,
    decay_param,
    channel_gain,
    out_proj,
    post_gain,
    post_gate,
    post_up,
    post_down,
):
    after_pre = feed_forward(tokens, pre_gain, pre_gate, pre_up, pre_down)
    after_mix = recurrent_mixer(
        after_pre,
        mix_gain,
        branch_proj,
        gate_proj,
        conv_taps,
        retain_blocks,
        admit_blocks,
        decay_param,
        channel_gain,
        out_proj,
    )
    return feed_forward(after_mix, post_gain, post_gate, post_up, post_down)


def solution(mesh):
    placed = (
        P("fs", "tp"),
        P(),
        P("fs", "tp"),
        P("fs", "tp"),
        P("fs", "tp"),
        P(),
        P("fs", "tp"),
        P("fs", "tp"),
        P(None, "tp"),
        P("tp", None, None),
        P("tp", None, None),
        P("tp"),
        P(),
        P("fs", "tp"),
        P(),
        P("fs", "tp"),
        P("fs", "tp"),
        P("fs", "tp"),
    )
    fs_size, tp_size = mesh.shape["fs"], mesh.shape["tp"]

    def layer(*arrays):
        if fits_fused(fs_size, tp_size, arrays):
            return fused(fs_size, tp_size, *arrays)
        return local(*arrays)

    return jax.shard_map(
        layer, mesh=mesh, in_specs=placed, out_specs=P("fs", "tp"), check_vma=False
    )
```
